32 devices in a mesh: grp: 2 (over y), ep: 4 (over z), tp: 4 (over x, core).
Axes of the slice: x: 2, y: 2, z: 4, core: 2. Of those that a mesh axis runs over, the one named last changes fastest.
Arguments:
- queries: bfloat16 [16384, 1024], P(('grp', 'ep'), 'tp'), parts along dimension 0, may hold values from -6 to 6
- key_vectors: bfloat16 [16384, 1024], P(('grp', 'ep'), 'tp'), parts along dimension 0, may hold values from -6 to 6
- value_vectors: bfloat16 [16384, 1024], P(('grp', 'ep'), 'tp'), parts along dimension 0, may hold values from -6 to 6
- input_gate: float32 [16384, 16], P(('grp', 'ep'), 'tp'), parts along dimension 0, may hold values from -6 to 320
- forget_gate: float32 [16384, 16], P(('grp', 'ep'), 'tp'), parts along dimension 0, may hold values from 0 to 15
- head_gain: float32 [1024], P('tp'), may hold values from 0.1 to 1.9
- out_weight: bfloat16 [1024, 2048], P(None, 'tp'), may hold values from -0.1875 to 0.1875
- expert_input: bfloat16 [1024, 2048], P(('grp', 'ep')), parts along dimension 0, may hold values from -6 to 6
- norm_gain: float32 [2048], replicated, may hold values from 0.1 to 1.9
- routes: int32 [1024, 2], P(('grp', 'ep')), parts along dimension 0, may hold values from 0 to 3, all different within a row; in each aligned block of 128 rows (0 to 127, 128 to 255, ...) at most 80 rows name the same one
- route_weight: float32 [1024, 2], P(('grp', 'ep')), parts along dimension 0, may hold values from 0.25 to 1
- gate_weight: bfloat16 [4, 2048, 3584], P('ep', None, 'tp'), may hold values from -0.125 to 0.125
- up_weight: bfloat16 [4, 2048, 3584], P('ep', None, 'tp'), may hold values from -0.125 to 0.125
- down_weight: bfloat16 [4, 3584, 2048], P('ep', 'tp'), may hold values from -0.125 to 0.125
Outputs:
- mixer_out: bfloat16 [16384, 2048], P(('grp', 'ep'), 'tp'), parts along dimension 0
- expert_out: bfloat16 [1024, 2048], P(('grp', 'ep'), 'tp'), parts along dimension 0
The draws below stay inside these ranges and needn't reach their ends.
There are 2 independent parts, one for each index of `grp`. The reference program is written for one: setup_inputs(seed, part) draws one part's arguments, and reference() takes and returns one part's arrays. A program takes and returns all parts, laid end to end along the dimension named above; an argument that names none is the same for every part. Nothing has to cross between parts.
Inputs may be any that keep to these rules, and one draw needn't show every extreme that they name: `routes`: A token's 2 experts differ. Among the 128 tokens of one index of ep, no expert is named more than 80 times, and in some of these blocks one is named exactly 80 times.
All inputs are finite; a program needn't handle non-finite values.
Results may differ from the reference program's by a relative error of at most 0.019.
Values may be sent and summed in bfloat16 or wider, within the bound.
A program may use at most 64 MiB of HBM per device.

```python
import math
import jax
import jax.numpy as jnp
import numpy as np
from jax import lax

D = 2048
MEMORY_HEADS = 16
HEAD = 64
FF = 3584
BLK = 128
TOP = 2
SEG = 2048
ROWS = 128
SEQUENCE_TOKENS = 8192
TOKENS_B = 512
EXPERTS = 4
CAP = 80
N_EP = 4
N_TP = 4


def draw_forget_gate(key, part):
    key_sequence = jax.random.split(jax.random.fold_in(key, 11), 5)
    chance = 0.5
    fast_head = jax.random.uniform(key_sequence[0], (MEMORY_HEADS,)) < chance
    base_rate = jnp.where(fast_head, 1.0 / 40.0, 0.25 / SEQUENCE_TOKENS)
    factor = jnp.exp(jax.random.uniform(key_sequence[1], (SEQUENCE_TOKENS // SEG, 1), minval=-0.7, maxval=0.7))
    factor = jnp.repeat(factor, SEG, axis=0)
    jitter = jnp.exp(0.5 * jnp.clip(jax.random.normal(key_sequence[2], (SEQUENCE_TOKENS, MEMORY_HEADS)), -3.0, 3.0))
    update_rate = base_rate[None, :] * factor * jitter
    surge_position = jax.random.randint(key_sequence[3], (2, MEMORY_HEADS), 0, SEQUENCE_TOKENS)
    token_position = jnp.arange(SEQUENCE_TOKENS)[:, None, None]
    surge_reached = jnp.any(token_position == surge_position[None], axis=1)
    surge_penalty = jax.random.uniform(key_sequence[4], (SEQUENCE_TOKENS, MEMORY_HEADS), minval=0.22, maxval=0.69)
    update_rate = jnp.where(surge_reached, surge_penalty, update_rate)
    return (-jnp.log(jnp.expm1(update_rate))).astype(jnp.float32)


def draw_input_gate(key, part):
    key_sequence = jax.random.split(jax.random.fold_in(key, 12), 1)
    gate_values = 1.5 * jnp.clip(jax.random.normal(key_sequence[0], (SEQUENCE_TOKENS, MEMORY_HEADS)), -4.0, 4.0)
    return gate_values.astype(jnp.float32)


def with_spikes(array, stream_key, source, target, blocks, factor):
    def block_of(position):
        return (jnp.arange(array.shape[position]) // (array.shape[position] // blocks)).reshape((-1,) + (1,) * (array.ndim - 1 - position))

    near = jax.random.permutation(stream_key, blocks)[block_of(target)]
    second = (block_of(target) + blocks // 2) % blocks
    return jnp.where((block_of(source) == near) | (block_of(source) == second), factor * array, array)


def shard_levels(own_key, shape, pieces, smallest, largest):
    def one(axis_at, parts):
        steps = jax.random.uniform(jax.random.fold_in(jax.random.fold_in(own_key, 6), axis_at), (parts,), jnp.float32, smallest / len(pieces), largest / len(pieces))
        return jnp.repeat(jnp.exp(steps), shape[axis_at] // parts).reshape((-1,) + (1,) * (len(shape) - axis_at - 1))

    loudness = one(*pieces[0])
    for cut in pieces[1:]:
        loudness = loudness * one(*cut)
    return loudness


def shared_out(rng, own, number, rows, count, top, most, skew):
    ranking = jax.random.permutation(rng, count)
    crowded, usual = shares(count, rows * top, most, skew, True), shares(count, rows * top, most, skew, False)
    places = jnp.arange(count)

    def named(lengths, rotation):
        used = int((lengths > 0).sum())
        fixed = max(1, used // 4)
        shifted = fixed + (places - fixed + rotation * (used - fixed)) % max(1, count - fixed)
        return jnp.zeros((count,), jnp.int32).at[ranking[jnp.where(places < fixed, places, shifted)]].set(jnp.asarray(lengths, jnp.int32))

    lengths = jnp.where(number % 4 == 0, named(crowded, number // 4), named(usual, number - number // 4 - 1))
    mixed = jax.random.permutation(jax.random.fold_in(own, 3), count)
    donor, sink = mixed[0:count // 2 * 2:2], mixed[1:count // 2 * 2:2]
    room = jnp.minimum(lengths[donor] - 1, most - lengths[sink]) // 2
    room = jnp.where((donor == ranking[0]) | (sink == ranking[0]) | (lengths[sink] == 0), 0, jnp.maximum(room, 0))
    shifted = jax.random.randint(jax.random.fold_in(own, 4), (count // 2,), 0, 1 << 20) % (room + 1)
    lengths = lengths.at[donor].add(-shifted).at[sink].add(shifted)
    items = jnp.searchsorted(jnp.cumsum(lengths), jnp.arange(rows * top), side="right").astype(jnp.int32)
    table = items.reshape(top, rows).T
    table = table[jax.random.permutation(jax.random.fold_in(own, 1), rows)]
    rotation = jax.random.randint(jax.random.fold_in(own, 2), (rows, 1), 0, top)
    return jnp.take_along_axis(table, (jnp.arange(top)[None, :] + rotation) % top, axis=1)


def shares(amount, total, limit, skew, full):
    loads = [(1 << 20) // math.isqrt(grade ** skew) + 1 for grade in range(1, amount + 1)]
    largest = limit if full else min(limit, max(-(-total // amount), total * loads[0] // sum(loads)))
    least = 1 if total - largest >= amount - 1 else 0
    given, rest = [largest] + [least] * (amount - 1), total - largest - least * (amount - 1)
    while rest > 0:
        free = [i for i in range(1, amount) if given[i] < largest] or [i for i in range(1, amount) if given[i] < limit]
        mass, remaining = sum([loads[i] for i in free]), rest
        for i in free:
            extra = min(limit - given[i], max(1, remaining * loads[i] // mass), rest)
            given[i] = given[i] + extra
            rest = rest - extra
    return np.array(given)


def bell_draw(key, extent, spread, most, shards=(), held_as=jnp.bfloat16):
    array = spread * jax.random.normal(key, extent, jnp.float32)
    if shards:
        array = array * shard_levels(key, extent, shards, -0.22, 0.18)
    return jnp.clip(array, -most, most).astype(held_as)


def bell_draw_with(stream_key, extent, width, reach, shards, heavy, kind=jnp.bfloat16):
    array = width * jax.random.normal(stream_key, extent, jnp.float32)
    if shards:
        array = array * shard_levels(stream_key, extent, shards, -0.22, 0.18)
    return jnp.clip(with_spikes(array, jax.random.fold_in(stream_key, 3), *heavy), -reach, reach).astype(kind)


def setup_inputs(seed: int = 0, part: int = 0) -> dict:
    arg_keys = jax.random.split(jax.random.key(seed), 15)
    part_keys = jax.random.split(jax.random.fold_in(arg_keys[14], part), 15)
    queries = bell_draw(part_keys[0], (SEQUENCE_TOKENS, MEMORY_HEADS * HEAD), 1.0, 6.0, ((0, 4), (1, 4)))
    key_vectors = bell_draw(part_keys[1], (SEQUENCE_TOKENS, MEMORY_HEADS * HEAD), 1.0, 6.0, ((0, 4), (1, 4)))
    value_vectors = bell_draw(part_keys[2], (SEQUENCE_TOKENS, MEMORY_HEADS * HEAD), 1.0, 6.0, ((0, 4), (1, 4)))
    input_gate = draw_input_gate(jax.random.fold_in(jax.random.fold_in(arg_keys[14], part), 71), part)
    forget_gate = draw_forget_gate(jax.random.fold_in(jax.random.fold_in(arg_keys[14], part), 71), part)
    head_gain = jnp.clip(1.0 + 0.18 * jax.random.normal(arg_keys[5], (MEMORY_HEADS * HEAD,), jnp.float32), 0.1, 1.9)
    out_weight = bell_draw(arg_keys[6], (MEMORY_HEADS * HEAD, D), (MEMORY_HEADS * HEAD) ** -0.5, 0.1875, ((1, 4),))
    expert_input = bell_draw(part_keys[7], (TOKENS_B, D), 1.0, 6.0, ((0, 4),))
    norm_gain = jnp.clip(1.0 + 0.18 * jax.random.normal(arg_keys[8], (D,), jnp.float32), 0.1, 1.9)
    routes_keys = jax.random.split(jax.random.fold_in(part_keys[9], 1), TOKENS_B // ROWS)
    routes_turns = jax.random.permutation(jax.random.fold_in(part_keys[9], 3), TOKENS_B // ROWS)
    routes = jax.vmap(lambda own, number: shared_out(jax.random.fold_in(part_keys[9], 2), own, number, ROWS, EXPERTS, TOP, CAP, 2))(routes_keys, routes_turns).reshape((TOKENS_B, TOP))
    route_weight = jnp.clip(0.25 + 0.75 * jax.random.uniform(part_keys[10], (TOKENS_B, TOP), jnp.float32) ** shard_levels(part_keys[10], (TOKENS_B, TOP), ((0, 4),), -0.2, 0.2), 0.25, 1.0)
    gate_weight = bell_draw(arg_keys[11], (EXPERTS, D, FF), D ** -0.5, 0.125, ((0, 4), (2, 4)))
    up_weight = bell_draw(arg_keys[12], (EXPERTS, D, FF), D ** -0.5, 0.125, ((0, 4), (2, 4)))
    down_weight = bell_draw_with(arg_keys[13], (EXPERTS, FF, D), FF ** -0.5, 0.125, ((0, 4), (1, 4)), (1, 2, 4, 2.0))
    return dict(queries=queries, key_vectors=key_vectors, value_vectors=value_vectors, input_gate=input_gate, forget_gate=forget_gate, head_gain=head_gain, out_weight=out_weight, expert_input=expert_input, norm_gain=norm_gain, routes=routes, route_weight=route_weight, gate_weight=gate_weight, up_weight=up_weight, down_weight=down_weight)


EXACT_PRECISION = lax.Precision.HIGHEST

def to_bfloat(values):
    return lax.optimization_barrier(values.astype(jnp.bfloat16)).astype(jnp.float32)

def head_blocks(matrix):
    return matrix.reshape(-1, BLK, MEMORY_HEADS, HEAD).transpose(2, 0, 1, 3).astype(jnp.float32)

def gate_blocks(matrix):
    return matrix.reshape(-1, BLK, MEMORY_HEADS).transpose(2, 0, 1)

def advance(carry, inputs):
    memory_matrix, normer_state, stable_state = carry
    block_end, tail_gate, key_block, block_values = inputs
    stable_next = jnp.maximum(block_end + stable_state, lax.optimization_barrier(jnp.max(tail_gate, axis=-1)))
    decay_factor = jnp.exp(block_end + stable_state - stable_next)
    key_weight = jnp.exp(tail_gate - stable_next[:, None])
    key_weighted_rows = to_bfloat(key_weight[..., None] * key_block)
    following_matrix = decay_factor[:, None, None] * memory_matrix + jnp.einsum('fjt,fjz->ftz', key_weighted_rows, block_values, precision=EXACT_PRECISION)
    normer_next = decay_factor[:, None] * normer_state + lax.optimization_barrier(jnp.sum(key_weighted_rows, axis=1))
    return ((following_matrix, normer_next, stable_next), (memory_matrix, normer_state, stable_state))

def head_cells(items):
    query_block, key_block, block_values, decay_sum, gate_in, matrix_in, normer_in, stable_in = items
    causal = jnp.arange(BLK)[:, None] >= jnp.arange(BLK)[None, :]
    log_weights = decay_sum[:, :, None] - decay_sum[:, None, :] + gate_in[:, None, :]
    log_weights = jnp.where(causal[None], log_weights, -jnp.inf)
    stabilizer = jnp.maximum(decay_sum + stable_in[:, None], lax.optimization_barrier(jnp.max(log_weights, axis=-1)))
    head_scale = HEAD ** (-0.5)
    scores = jnp.einsum('cjd,csd->cjs', query_block, key_block, precision=EXACT_PRECISION) * head_scale
    weighted = jnp.exp(log_weights - stabilizer[..., None]) * scores
    weighted_b = to_bfloat(weighted)
    carried_scale = jnp.exp(decay_sum + stable_in[:, None] - stabilizer)
    carried = jnp.einsum('cjk,ckv->cjv', query_block, matrix_in, precision=EXACT_PRECISION) * head_scale
    numerator = carried_scale[..., None] * carried + jnp.einsum('cjs,csv->cjv', weighted_b, block_values, precision=EXACT_PRECISION)
    denominator = carried_scale * jnp.einsum('cjk,ck->cj', query_block, normer_in, precision=EXACT_PRECISION) * head_scale + lax.optimization_barrier(jnp.sum(weighted, axis=-1))
    return numerator / jnp.maximum(jnp.abs(denominator), jnp.exp(-stabilizer))[..., None]

def expert_block(items):
    rows_in, gate_mat, up_mat, down_mat = items
    gate_act = jnp.dot(rows_in, gate_mat, preferred_element_type=jnp.float32)
    up_act = jnp.dot(rows_in, up_mat, preferred_element_type=jnp.float32)
    hidden = (jax.nn.silu(gate_act) * up_act).astype(jnp.bfloat16)
    group_width = FF // N_TP
    hidden_groups = hidden.reshape(-1, N_TP, group_width).astype(jnp.float32)
    down_groups = down_mat.reshape(N_TP, group_width, D).astype(jnp.float32)
    piece_sum = jnp.einsum('rgf,gfd->grd', hidden_groups, down_groups, precision=EXACT_PRECISION)
    piece_sum = to_bfloat(piece_sum)
    return lax.optimization_barrier(jnp.sum(piece_sum, axis=0)).astype(jnp.bfloat16)

def reference(queries, key_vectors, value_vectors, input_gate, forget_gate, head_gain, out_weight, expert_input, norm_gain, routes, route_weight, gate_weight, up_weight, down_weight):
    query_all = head_blocks(queries)
    key_all = head_blocks(key_vectors)
    value_all = head_blocks(value_vectors)
    gate_all = gate_blocks(input_gate)
    logf = gate_blocks(jax.nn.log_sigmoid(forget_gate))
    decay_sum = jnp.cumsum(logf, axis=-1)
    block_end = decay_sum[..., -1]
    tail_gate = block_end[..., None] - decay_sum + gate_all
    initial = (jnp.zeros((MEMORY_HEADS, HEAD, HEAD), jnp.float32), jnp.zeros((MEMORY_HEADS, HEAD), jnp.float32), jnp.zeros((MEMORY_HEADS,), jnp.float32))
    inputs = (jnp.moveaxis(block_end, 1, 0), jnp.moveaxis(tail_gate, 1, 0), jnp.moveaxis(key_all, 1, 0), jnp.moveaxis(value_all, 1, 0))
    ignored, entering = lax.scan(advance, initial, inputs)
    matrix_in, normer_in, stable_in = [jnp.moveaxis(part, 0, 1) for part in entering]
    cells = lax.map(head_cells, (query_all, key_all, value_all, decay_sum, gate_all, matrix_in, normer_in, stable_in))
    normed = cells * lax.rsqrt(lax.optimization_barrier(jnp.mean(cells * cells, axis=-1, keepdims=True)) + 1e-06)
    normed = (normed * head_gain.reshape(MEMORY_HEADS, 1, 1, HEAD)).astype(jnp.bfloat16)
    normed = normed.transpose(1, 2, 0, 3).reshape(-1, MEMORY_HEADS * HEAD)
    mixer_out = jnp.dot(normed, out_weight, preferred_element_type=jnp.float32).astype(jnp.bfloat16)
    input_wide = expert_input.astype(jnp.float32)
    scaled = input_wide * lax.rsqrt(lax.optimization_barrier(jnp.mean(input_wide * input_wide, axis=-1, keepdims=True)) + 1e-06)
    scaled = (scaled * norm_gain).astype(jnp.bfloat16)
    chosen = routes.reshape(N_EP, ROWS * TOP)
    onehot = (chosen[..., None] == jnp.arange(EXPERTS, dtype=jnp.int32)[None, None, :]).astype(jnp.int32)
    slot_index = lax.optimization_barrier(jnp.sum((jnp.cumsum(onehot, axis=1) - onehot) * onehot, axis=-1))
    block_index = jnp.arange(N_EP, dtype=jnp.int32)[:, None]
    target = (chosen * (N_EP * CAP) + block_index * CAP + slot_index).reshape(-1).astype(jnp.int32)
    source = jnp.repeat(jnp.arange(TOKENS_B, dtype=jnp.int32), TOP)
    buffer = jnp.zeros((EXPERTS * N_EP * CAP, D), jnp.bfloat16).at[target].set(scaled[source])
    buffer = buffer.reshape(EXPERTS, N_EP * CAP, D)
    results = lax.map(expert_block, (buffer, gate_weight, up_weight, down_weight)).reshape(-1, D)
    copies = results[target].astype(jnp.float32).reshape(TOKENS_B, TOP, D)
    expert_out = lax.optimization_barrier(jnp.sum(copies * route_weight[..., None], axis=1)).astype(jnp.bfloat16)
    return (mixer_out, expert_out)
```

```python
import jax
import jax.numpy as jnp
from jax import lax
from jax.experimental import pallas as pl
from jax.experimental.pallas import tpu as pltpu
from jax.sharding import PartitionSpec as P

HEAD = 64
BLK = 128


EXACT_PRECISION = lax.Precision.HIGHEST
VERY_NEGATIVE = -1e30


def prefix(part, axis, combine, identity):
    place = lax.axis_index(axis)
    gathered = jax.tree.map(lambda a: lax.all_gather(a, axis), part)
    state = jax.tree.map(lambda a, e: jnp.zeros_like(a) + jnp.asarray(e, a.dtype), part, identity)

    def one(step, state):
        return combine(
            state, jax.tree.map(lambda a: lax.dynamic_index_in_dim(a, step, 0, False), gathered)
        )

    return lax.fori_loop(0, place, one, state)


def combine_states(before_part, after_part):
    decay_early, matrix_early, normer_early, stable_early = before_part
    decay_late, matrix_late, normer_late, stable_late = after_part
    highest = jnp.maximum(decay_late + stable_early, stable_late)
    scale_early = jnp.exp(decay_late + stable_early - highest)
    scale_late = jnp.exp(stable_late - highest)
    matrix_joined = (
        scale_early[..., None, None] * matrix_early + scale_late[..., None, None] * matrix_late
    )
    normer_joined = scale_early[..., None] * normer_early + scale_late[..., None] * normer_late
    return (decay_early + decay_late, matrix_joined, normer_joined, highest)


def memory_cells(queries, key_vectors, value_vectors, input_gate, forget_gate, head_gain):
    segment_len = input_gate.shape[0]
    heads = input_gate.shape[1]
    blocks = segment_len // BLK
    head_scale = HEAD ** (-0.5)

    def block_view(matrix):
        return matrix.reshape(blocks, BLK, heads, HEAD).transpose(2, 0, 1, 3)

    query_blocks = block_view(queries)
    key_blocks = block_view(key_vectors)
    value_blocks = block_view(value_vectors)
    input_blocks = input_gate.reshape(blocks, BLK, heads).transpose(2, 0, 1)
    log_forget = jax.nn.log_sigmoid(forget_gate).reshape(blocks, BLK, heads).transpose(2, 0, 1)
    running_decay = jnp.cumsum(log_forget, axis=-1)
    block_end = running_decay[..., -1]
    tail_gate = block_end[..., None] - running_decay + input_blocks
    block_peak = jnp.max(tail_gate, axis=-1)
    key_weight = jnp.exp(tail_gate - block_peak[..., None])
    key_weighted_rows = (key_weight[..., None] * key_blocks).astype(jnp.bfloat16)
    matrix_terms = jnp.einsum(
        "hcsk,hcsv->hckv", key_weighted_rows, value_blocks, preferred_element_type=jnp.float32
    )
    normer_terms = jnp.sum(key_weighted_rows.astype(jnp.float32), axis=2)
    inclusive = lax.associative_scan(
        combine_states, (block_end, matrix_terms, normer_terms, block_peak), axis=1
    )
    device_total = tuple((member[:, -1] for member in inclusive))
    identity = (
        jnp.zeros((heads,), jnp.float32),
        jnp.zeros((heads, HEAD, HEAD), jnp.float32),
        jnp.zeros((heads, HEAD), jnp.float32),
        jnp.full((heads,), VERY_NEGATIVE, jnp.float32),
    )
    earlier_states = prefix(device_total, "ep", combine_states, identity)
    initial = (
        jnp.zeros((heads,), jnp.float32),
        jnp.zeros((heads, HEAD, HEAD), jnp.float32),
        jnp.zeros((heads, HEAD), jnp.float32),
        jnp.zeros((heads,), jnp.float32),
    )
    entering = combine_states(initial, earlier_states)
    local_entry = tuple(
        (
            jnp.concatenate([start_value[:, None], member[:, :-1]], axis=1)
            for start_value, member in zip(identity, inclusive)
        )
    )
    incoming = tuple((member[:, None] for member in entering))
    ignored, matrix_entry, normer_entry, stable_entry = combine_states(incoming, local_entry)
    causal = jnp.arange(BLK)[:, None] >= jnp.arange(BLK)[None, :]
    log_weights = (
        running_decay[..., :, None] - running_decay[..., None, :] + input_blocks[..., None, :]
    )
    log_weights = jnp.where(causal, log_weights, -jnp.inf)
    stabilizer = jnp.maximum(running_decay + stable_entry[..., None], jnp.max(log_weights, axis=-1))
    scores = (
        jnp.einsum("hcjd,hcsd->hcjs", query_blocks, key_blocks, preferred_element_type=jnp.float32)
        * head_scale
    )
    weighted = jnp.exp(log_weights - stabilizer[..., None]) * scores
    carried_scale = jnp.exp(running_decay + stable_entry[..., None] - stabilizer)
    query_wide = query_blocks.astype(jnp.float32)
    carried = (
        jnp.einsum("hcjk,hckv->hcjv", query_wide, matrix_entry, precision=EXACT_PRECISION)
        * head_scale
    )
    numerator = carried_scale[..., None] * carried + jnp.einsum(
        "hcjs,hcsv->hcjv",
        weighted.astype(jnp.bfloat16),
        value_blocks,
        preferred_element_type=jnp.float32,
    )
    denominator = carried_scale * jnp.einsum(
        "hcjk,hck->hcj", query_wide, normer_entry, precision=EXACT_PRECISION
    ) * head_scale + jnp.sum(weighted, axis=-1)
    cells = numerator / jnp.maximum(jnp.abs(denominator), jnp.exp(-stabilizer))[..., None]
    normed = cells * lax.rsqrt(jnp.mean(cells * cells, axis=-1, keepdims=True) + 1e-06)
    normed = (normed * head_gain.reshape(heads, 1, 1, HEAD)).astype(jnp.bfloat16)
    return normed.transpose(1, 2, 0, 3).reshape(segment_len, heads * HEAD)


def mm(a, b, ca, cb, precision=None):
    return lax.dot_general(
        a, b, (((ca,), (cb,)), ((), ())), preferred_element_type=jnp.float32, precision=precision
    )


def iota(shape, axis):
    return lax.broadcasted_iota(jnp.int32, shape, axis)


def split_parts(x, count):
    parts = []
    for _ in range(count):
        part = x.astype(jnp.bfloat16)
        parts.append(part.astype(jnp.float32))
        x = x - part.astype(jnp.float32)
    return jnp.concatenate(parts, axis=0).astype(jnp.bfloat16)


def lane_heads(rows, width):
    own = iota((rows, width), 1) // HEAD == iota((rows, width), 0) % 8
    return jnp.where(own, 1.0, 0.0)


def spread_columns(rows8, count, width):
    return mm(split_parts(rows8, count), lane_heads(8 * count, width).astype(jnp.bfloat16), 0, 0)


def spread_lanes(rows8, width):
    wide = jnp.concatenate([rows8] * (width // rows8.shape[1]), axis=1)
    return jnp.sum(wide * lane_heads(8, width), axis=0, keepdims=True)


def diagonal(width):
    shape = (2 * HEAD, width)
    return iota(shape, 0) // HEAD == (iota(shape, 1) % (2 * HEAD)) // HEAD


def with_ones(v):
    return jnp.concatenate([v, jnp.ones_like(v)], axis=1)


def gate_prepare(fg, ig, decay_ref, g_ref):
    logf = jnp.minimum(fg, 0.0) - jnp.log1p(jnp.exp(-jnp.abs(fg)))
    upper = jnp.where(iota((BLK, BLK), 0) <= iota((BLK, BLK), 1), 1.0, 0.0)
    decay = mm(logf, upper, 1, 0, EXACT_PRECISION)
    g = ig - decay
    blocks = fg.shape[0] // 8
    decay_ref[...] = decay.reshape(blocks, 8, BLK)
    g_ref[...] = g.reshape(blocks, 8, BLK)
    return decay, g


def device_state(k_ref, v_ref, fg, ig, decay_ref, g_ref, kw_ref, acc_ref):
    decay, g = gate_prepare(fg, ig, decay_ref, g_ref)
    rows = fg.shape[0]
    blocks = rows // 8
    width = k_ref.shape[1]
    ends = jnp.broadcast_to(decay[:, BLK - 1 : BLK], (rows, BLK))
    here, there = iota((rows, rows), 0), iota((rows, rows), 1)
    earlier = (here % 8 == there % 8) & (there // 8 < here // 8)
    before = mm(jnp.where(earlier, 1.0, 0.0), ends, 1, 0, EXACT_PRECISION)
    total = (before + ends)[rows - 8 :]
    shifted = (g - before).reshape(blocks, 8, BLK)
    highest = jnp.max(jnp.max(shifted, axis=0), axis=-1, keepdims=True)
    highest = jnp.broadcast_to(highest, (8, BLK))
    kw_ref[...] = jnp.exp(shifted - highest[None])
    acc_ref[...] = jnp.zeros_like(acc_ref)

    def one(b, carry):
        at = pl.ds(pl.multiple_of(b * BLK, BLK), BLK)
        keys = spread_columns(kw_ref[b], 2, width) * k_ref[at, :].astype(jnp.float32)
        keys = keys.astype(jnp.bfloat16)
        for p in range(width // (2 * HEAD)):
            cols = slice(2 * HEAD * p, 2 * HEAD * (p + 1))
            acc_ref[p] += mm(keys[:, cols], with_ones(v_ref[at, cols]), 0, 0)
        return carry

    lax.fori_loop(0, blocks, one, 0, unroll=2)
    return total, total + highest


def folded(state):
    state = jnp.where(diagonal(state.shape[1]), state, 0.0)
    return state[:HEAD] + state[HEAD:]


def unfolded(half):
    both = jnp.concatenate([half, half], axis=0)
    return jnp.where(diagonal(half.shape[1]), both, 0.0)


def cell_block(b, q_ref, k_ref, v_ref, decay_ref, g_ref, gain, state_ref, m_ref):
    at = pl.ds(pl.multiple_of(b * BLK, BLK), BLK)
    width = q_ref.shape[1]
    pair = 2 * HEAD
    g, decay, m = g_ref[b], decay_ref[b], m_ref[...]
    causal = iota((BLK, BLK), 0) >= iota((BLK, BLK), 1)
    low = iota((BLK, pair), 1) < HEAD
    decay_wide = spread_columns(decay, 3, width)
    peak = jnp.maximum(m, jnp.broadcast_to(jnp.max(g, axis=-1, keepdims=True), g.shape))
    keys_scale = spread_columns(jnp.exp(g - peak), 2, width)
    m_wide = spread_lanes(m, width)
    keep = spread_lanes(jnp.exp(m - peak), width)
    m_ref[...] = peak + jnp.broadcast_to(decay[:, BLK - 1 : BLK], g.shape)
    mean = jnp.where(diagonal(pair), 1.0 / HEAD, 0.0).astype(jnp.bfloat16)
    out = []
    for p in range(width // pair):
        cols = slice(pair * p, pair * (p + 1))
        kp = k_ref[at, cols]
        vp = with_ones(v_ref[at, cols])
        qf = q_ref[at, cols].astype(jnp.float32) * HEAD ** (-0.5)
        tops, sums = [], []
        for i in range(2):
            h = 2 * p + i
            qm = jnp.where(low if i == 0 else ~low, qf, 0.0).astype(jnp.bfloat16)
            scores = mm(qm, kp, 1, 1)
            gm = jnp.where(causal, g[h : h + 1, :], VERY_NEGATIVE)
            top = jnp.maximum(jnp.max(gm, axis=-1, keepdims=True), m[h : h + 1, 0:1])
            weighted = jnp.exp(gm - top) * scores
            tops.append(top)
            sums.append(mm(weighted.astype(jnp.bfloat16), vp, 1, 0))
        top = jnp.where(low, tops[0], tops[1])
        carried_scale = jnp.exp(m_wide[:, cols] - top)
        state = state_ref[p]
        carried = mm((qf * carried_scale).astype(jnp.bfloat16), state.astype(jnp.bfloat16), 1, 0)
        num = jnp.where(low, sums[0][:, :pair], sums[1][:, :pair]) + carried[:, :pair]
        den = jnp.where(low, sums[0][:, pair:], sums[1][:, pair:]) + carried[:, pair:]
        floor = jnp.exp(-(decay_wide[:, cols] + top))
        cells = num / jnp.maximum(jnp.abs(den), floor)
        square = mm((cells * cells).astype(jnp.bfloat16), mean, 1, 0)
        normed = cells * lax.rsqrt(square + 1e-06) * gain[:, cols]
        out.append(normed.astype(jnp.bfloat16))
        keys = (keys_scale[:, cols] * kp.astype(jnp.float32)).astype(jnp.bfloat16)
        fresh = jnp.where(diagonal(2 * pair), mm(keys, vp, 0, 0), 0.0)
        kept = keep[:, cols]
        state_ref[p] = jnp.concatenate([kept, kept], axis=1) * state + fresh
    return jnp.concatenate(out, axis=1)


def joined(early, late, take):
    mats, m = early
    late_mats, late_decay, late_m = late
    top = jnp.maximum(late_decay + m, late_m)
    width = 2 * HEAD * len(mats)
    old = spread_lanes(jnp.exp(late_decay + m - top), width)
    new = spread_lanes(jnp.exp(late_m - top), width)
    result = []
    for p, mat in enumerate(mats):
        cols = slice(2 * HEAD * p, 2 * HEAD * (p + 1))
        s0 = jnp.concatenate([old[:, cols]] * 2, axis=1)
        s1 = jnp.concatenate([new[:, cols]] * 2, axis=1)
        result.append(jnp.where(take, s0 * mat + s1 * late_mats[p].astype(jnp.float32), mat))
    return result, jnp.where(take, top, m)


def gates_by_block(gates):
    length, heads = gates.shape
    rows = jnp.pad(gates, ((0, 0), (0, 8 - heads))).reshape(length // BLK, BLK, 8)
    return rows.transpose(0, 2, 1).reshape(length // BLK * 8, BLK)


MESH = pl.DeviceIdType.MESH


def layer_kernel(
    q_ref, k_ref, v_ref, fg_ref, ig_ref, gain_ref, x_ref, xgain_ref, routes_ref, across_ref, share_ref,
    gate_ref, up_ref, down_ref, project_ref, mixer_ref, expert_ref,
    decay, g, kw, acc, m, every_mats, every_marks, outgoing, flat, gate_up, down, project, hidden,
    piece, near, far_out, far_in, copied, returned, normed,
    load_sem, dispatch_sem, join_sem, mats_sem, marks_sem, near_sem, far_sem, return_sem, cross_sem, side_sem, pass_sem,
):
    ep, place = lax.axis_size("ep"), lax.axis_index("ep")
    tp = lax.axis_index("tp")
    core, chip = lax.rem(tp, 2), lax.div(tp, 2)
    sibling, opposite = chip * 2 + (1 - core), (1 - chip) * 2 + core
    tokens, choices = routes_ref.shape
    capacity, half = outgoing.shape[1:]
    pairs = acc.shape[0]
    piece_width = piece.shape[2]
    tile = gate_up.shape[2] // 2
    tiles = gate_up.shape[0]

    def remote(src, dst, sems, index, device):
        return pltpu.make_async_remote_copy(
            src_ref=src, dst_ref=dst, send_sem=sems.at[0, index], recv_sem=sems.at[1, index],
            device_id=device, device_id_type=MESH,
        )

    def tile_load(source, n, side):
        return pltpu.make_async_copy(
            source.at[:, pl.ds(pl.multiple_of(n * tile, tile), tile)],
            gate_up.at[n, :, pl.ds(side * tile, tile)],
            load_sem.at[side, n],
        )

    down_load = pltpu.make_async_copy(down_ref, down, load_sem.at[0, tiles])
    project_load = pltpu.make_async_copy(project_ref, project, load_sem.at[1, tiles])

    barrier = pltpu.get_barrier_semaphore()
    partners = [{"ep": lax.rem(place + d, ep)} for d in range(1, ep)] + [{"tp": sibling}, {"tp": opposite}]
    for partner in partners:
        pl.semaphore_signal(barrier, inc=1, device_id=partner, device_id_type=MESH)

    def start_tile(n, carry):
        tile_load(gate_ref, n, 0).start()
        tile_load(up_ref, n, 1).start()
        return carry

    lax.fori_loop(0, tiles, start_tile, 0)
    down_load.start()
    project_load.start()

    wide = x_ref[...].astype(jnp.float32)
    inverse = lax.rsqrt(jnp.mean(wide * wide, axis=-1, keepdims=True) + 1e-06)
    mine = pl.ds(pl.multiple_of(core * half, half), half)
    narrow = (x_ref[:, mine].astype(jnp.float32) * inverse * xgain_ref[:, mine]).astype(jnp.bfloat16)
    order = iota((tokens, tokens), 0) < iota((tokens, tokens), 1)
    order = jnp.where(order, 1.0, 0.0).astype(jnp.bfloat16)

    def rows_for(expert):
        named = jnp.zeros((8, tokens), jnp.float32)
        for k in range(choices):
            named += jnp.where(across_ref[k : k + 1, :] == expert, 1.0, 0.0)
        slot = mm(named.astype(jnp.bfloat16), order, 1, 0)
        chosen = (slot[0:1] == iota((capacity, tokens), 0).astype(jnp.float32)) & (named[0:1] > 0.5)
        pick = jnp.where(chosen, 1.0, 0.0).astype(jnp.bfloat16)
        return mm(pick, narrow, 1, 0).astype(jnp.bfloat16)

    for d in range(1, ep):
        outgoing[d - 1] = rows_for(lax.rem(place + d, ep))
    flat[core, place] = rows_for(place)
    pl.semaphore_wait(barrier, len(partners))
    dispatches = [
        remote(outgoing.at[d - 1], flat.at[core, place], dispatch_sem, d - 1, {"ep": lax.rem(place + d, ep)})
        for d in range(1, ep)
    ]
    for copy in dispatches:
        copy.start()

    total, top = device_state(k_ref, v_ref, fg_ref[...], ig_ref[...], decay, g, kw, acc)
    for p in range(pairs):
        every_mats[place, p] = folded(acc[p]).astype(jnp.bfloat16)
    every_marks[place] = jnp.concatenate([total, top], axis=1)

    for copy in dispatches:
        copy.wait_recv()
    join = remote(flat.at[core], flat.at[core], join_sem, 0, {"tp": sibling})
    join.start()
    states = []
    for d in range(1, ep):
        peer = {"ep": lax.rem(place + d, ep)}
        states.append(remote(every_mats.at[place], every_mats.at[place], mats_sem, d - 1, peer))
        states.append(remote(every_marks.at[place], every_marks.at[place], marks_sem, d - 1, peer))
    for copy in states:
        copy.start()
    join.wait_recv()

    rows = ep * capacity

    def hidden_tile(n, carry):
        tile_load(gate_ref, n, 0).wait()
        tile_load(up_ref, n, 1).wait()
        both = mm(flat[0].reshape(rows, half), gate_up[n, :half, :], 1, 0)
        both += mm(flat[1].reshape(rows, half), gate_up[n, half:, :], 1, 0)
        gate_act, up_act = both[:, :tile], both[:, tile:]
        result = gate_act / (1.0 + jnp.exp(-gate_act)) * up_act
        hidden[:, pl.ds(pl.multiple_of(n * tile, tile), tile)] = result.astype(jnp.bfloat16)
        return carry

    lax.fori_loop(0, tiles, hidden_tile, 0)
    down_load.wait()

    def down_piece(slot, owner):
        cols = pl.ds(pl.multiple_of(owner * piece_width, piece_width), piece_width)
        piece[slot] = mm(hidden[...], down[:, cols], 1, 0).astype(jnp.bfloat16)

    near_copies = [remote(piece.at[i], near.at[i], near_sem, i, {"tp": sibling}) for i in range(2)]
    down_piece(0, (1 - chip) * 2 + (1 - core))
    near_copies[0].start()
    down_piece(1, sibling)
    near_copies[1].start()
    down_piece(2, opposite)
    near_copies[0].wait_recv()
    joint = piece[2].astype(jnp.float32) + near[0].astype(jnp.float32)
    far_out[...] = joint.astype(jnp.bfloat16)
    far_copy = remote(far_out, far_in, far_sem, 0, {"tp": opposite})
    far_copy.start()
    down_piece(3, tp)

    for copy in states:
        copy.wait_recv()
    held = ([jnp.zeros((HEAD, 4 * HEAD), jnp.float32)] * pairs, jnp.zeros((8, BLK), jnp.float32))
    for j in range(ep):
        marks = every_marks[j]
        late = ([every_mats[j, p] for p in range(pairs)], marks[:, :BLK], marks[:, BLK:])
        held = joined(held, late, j < place)
    for p in range(pairs):
        acc[p] = unfolded(held[0][p])
    m[...] = held[1]
    gain = gain_ref[...]

    groups = cross_sem.shape[1]
    group_rows = q_ref.shape[0] // groups
    per_group = group_rows // BLK
    cross, side, onward = [], [], []
    for n in range(groups):
        span = pl.ds(n * group_rows, group_rows)
        own, other = normed.at[tp, span, :], normed.at[opposite, span, :]
        cross.append(remote(own, own, cross_sem, n, {"tp": opposite}))
        side.append(remote(own, own, side_sem, n, {"tp": sibling}))
        onward.append(remote(other, other, pass_sem, n, {"tp": sibling}))

    def one(b, carry):
        at = pl.ds(pl.multiple_of(b * BLK, BLK), BLK)
        normed[tp, at, :] = cell_block(b, q_ref, k_ref, v_ref, decay, g, gain, acc, m)
        return carry

    returns = [
        remote(copied.at[lax.rem(place + d, ep)], returned.at[place], return_sem, d - 1, {"ep": lax.rem(place + d, ep)})
        for d in range(1, ep)
    ]
    for n in range(groups):
        lax.fori_loop(n * per_group, (n + 1) * per_group, one, 0)
        cross[n].start()
        side[n].start()
        if n == groups // 2:
            near_copies[1].wait_recv()
            far_copy.wait_recv()
            summed = piece[3].astype(jnp.float32) + near[1].astype(jnp.float32) + far_in[...].astype(jnp.float32)
            copied[...] = summed.astype(jnp.bfloat16).reshape(copied.shape)
            returned[place] = copied[place]
            for copy in returns:
                copy.start()
        if n >= groups // 2:
            cross[n - groups // 2].wait_recv()
            onward[n - groups // 2].start()

    for copy in returns:
        copy.wait_recv()
    before = iota((tokens, tokens), 1) < iota((tokens, tokens), 0)
    before = jnp.where(before, 1.0, 0.0).astype(jnp.bfloat16)
    result = jnp.zeros((tokens, piece_width), jnp.float32)
    for e in range(ep):
        named = jnp.zeros((tokens, 1), jnp.float32)
        weight = jnp.zeros((tokens, 1), jnp.float32)
        for k in range(choices):
            same = routes_ref[:, k : k + 1] == e
            named += jnp.where(same, 1.0, 0.0)
            weight += jnp.where(same, share_ref[:, k : k + 1], 0.0)
        named = jnp.broadcast_to(named, (tokens, capacity))
        slot = mm(before, named.astype(jnp.bfloat16), 1, 0)
        chosen = (slot == iota((tokens, capacity), 1).astype(jnp.float32)) & (named > 0.5)
        pick = jnp.where(chosen, weight, 0.0)
        coarse = pick.astype(jnp.bfloat16)
        fine = (pick - coarse.astype(jnp.float32)).astype(jnp.bfloat16)
        result += mm(coarse, returned[e], 1, 0) + mm(fine, returned[e], 1, 0)
    expert_ref[...] = result.astype(jnp.bfloat16)

    project_load.wait()
    sub = 2 * BLK
    for n in range(groups):
        if n >= groups - groups // 2:
            cross[n].wait_recv()
            onward[n].start()
        side[n].wait_recv()
        onward[n].wait_recv()

        def mixed(i, carry):
            at = pl.ds(pl.multiple_of(i * sub, sub), sub)
            sums = None
            for t in range(normed.shape[0]):
                term = mm(normed[t, at, :], project[t * normed.shape[2] : (t + 1) * normed.shape[2], :], 1, 0)
                sums = term if sums is None else sums + term
            mixer_ref[at, :] = sums.astype(jnp.bfloat16)
            return carry

        lax.fori_loop(n * group_rows // sub, (n + 1) * group_rows // sub, mixed, 0)

    for copy in dispatches + [join] + states + near_copies + [far_copy] + returns + cross + side + onward:
        copy.wait_send()


def whole_layer(
    queries, key_vectors, value_vectors, input_gate, forget_gate, head_gain, out_weight, expert_input,
    norm_gain, routes, route_weight, gate_weight, up_weight, down_weight,
):
    length, width = queries.shape
    blocks, pairs = length // BLK, width // (2 * HEAD)
    ep, tps = lax.axis_size("ep"), lax.axis_size("tp")
    tokens, choices = routes.shape
    features, units = gate_weight.shape[1:]
    capacity = 5 * tokens * choices // (4 * ep)
    capacity = -(-capacity // 16) * 16
    half, tile, groups = features // 2, BLK, 4
    piece_width = features // tps
    tiles = units // tile
    f32, bf16 = jnp.float32, jnp.bfloat16
    rows = pltpu.VMEM((blocks, 8, BLK), f32)
    sems = lambda n: pltpu.SemaphoreType.DMA((2, n))
    vmem, anywhere = pl.BlockSpec(memory_space=pltpu.VMEM), pl.BlockSpec(memory_space=pl.ANY)
    return pl.pallas_call(
        layer_kernel,
        out_shape=(
            jax.ShapeDtypeStruct((length, out_weight.shape[1]), bf16),
            jax.ShapeDtypeStruct((tokens, piece_width), bf16),
        ),
        in_specs=[vmem] * 11 + [anywhere] * 4,
        out_specs=(vmem, vmem),
        scratch_shapes=[
            rows,
            rows,
            rows,
            pltpu.VMEM((pairs, 2 * HEAD, 4 * HEAD), f32),
            pltpu.VMEM((8, BLK), f32),
            pltpu.VMEM((ep, pairs, HEAD, 4 * HEAD), bf16),
            pltpu.VMEM((ep, 8, 2 * BLK), f32),
            pltpu.VMEM((ep - 1, capacity, half), bf16),
            pltpu.VMEM((2, ep, capacity, half), bf16),
            pltpu.VMEM((tiles, features, 2 * tile), bf16),
            pltpu.VMEM((units, features), bf16),
            pltpu.VMEM(out_weight.shape, bf16),
            pltpu.VMEM((ep * capacity, units), bf16),
            pltpu.VMEM((4, ep * capacity, piece_width), bf16),
            pltpu.VMEM((2, ep * capacity, piece_width), bf16),
            pltpu.VMEM((ep * capacity, piece_width), bf16),
            pltpu.VMEM((ep * capacity, piece_width), bf16),
            pltpu.VMEM((ep, capacity, piece_width), bf16),
            pltpu.VMEM((ep, capacity, piece_width), bf16),
            pltpu.VMEM((tps, length, width), bf16),
            sems(tiles + 1),
            sems(ep - 1),
            sems(1),
            sems(ep - 1),
            sems(ep - 1),
            sems(2),
            sems(1),
            sems(ep - 1),
            sems(groups),
            sems(groups),
            sems(groups),
        ],
        compiler_params=pltpu.CompilerParams(
            collective_id=0, has_side_effects=True, vmem_limit_bytes=60 * 1024 * 1024
        ),
    )(
        queries,
        key_vectors,
        value_vectors,
        gates_by_block(forget_gate),
        gates_by_block(input_gate),
        head_gain.reshape(1, width),
        expert_input,
        norm_gain.reshape(1, features),
        routes,
        routes.T,
        route_weight,
        gate_weight[0],
        up_weight[0],
        down_weight[0],
        out_weight,
    )


def fits_one_kernel(queries, routes, gate_weight):
    ep, tps = lax.axis_size("ep"), lax.axis_size("tp")
    length, width = queries.shape
    return (
        tps == 4
        and ep > 1
        and width % (2 * HEAD) == 0
        and length % (8 * BLK) == 0
        and routes.shape[0] % BLK == 0
        and gate_weight.shape[2] % BLK == 0
    )


def on_device(
    queries,
    key_vectors,
    value_vectors,
    input_gate,
    forget_gate,
    head_gain,
    out_weight,
    expert_input,
    norm_gain,
    routes,
    route_weight,
    gate_weight,
    up_weight,
    down_weight,
):
    if fits_one_kernel(queries, routes, gate_weight):
        return whole_layer(
            queries,
            key_vectors,
            value_vectors,
            input_gate,
            forget_gate,
            head_gain,
            out_weight,
            expert_input,
            norm_gain,
            routes,
            route_weight,
            gate_weight,
            up_weight,
            down_weight,
        )
    normed = memory_cells(queries, key_vectors, value_vectors, input_gate, forget_gate, head_gain)
    mixer_out = jnp.dot(
        lax.all_gather(normed, "tp", axis=1, tiled=True),
        out_weight,
        preferred_element_type=jnp.float32,
    ).astype(jnp.bfloat16)
    tokens = expert_input.shape[0]
    row_width = expert_input.shape[1]
    choices_per = routes.shape[1]
    experts = lax.axis_size("ep")
    splits = lax.axis_size("tp")
    slice_width = row_width // splits
    capacity = 5 * tokens * choices_per // (4 * experts)
    input_wide = expert_input.astype(jnp.float32)
    scaled = input_wide * lax.rsqrt(
        jnp.mean(input_wide * input_wide, axis=-1, keepdims=True) + 1e-06
    )
    scaled = scaled * norm_gain
    chosen = routes.reshape(-1)
    onehot = (chosen[:, None] == jnp.arange(experts, dtype=jnp.int32)[None, :]).astype(jnp.int32)
    slot_index = jnp.sum((jnp.cumsum(onehot, axis=0) - onehot) * onehot, axis=1)
    target = chosen * capacity + slot_index
    source = jnp.repeat(jnp.arange(tokens, dtype=jnp.int32), choices_per)
    column_start = lax.axis_index("tp") * slice_width
    narrow = lax.dynamic_slice_in_dim(scaled, column_start, slice_width, 1).astype(jnp.bfloat16)
    outgoing = (
        jnp.zeros((experts * capacity, slice_width), jnp.bfloat16).at[target].set(narrow[source])
    )
    arrived = lax.all_to_all(
        outgoing.reshape(experts, capacity, slice_width),
        "ep",
        split_axis=0,
        concat_axis=0,
        tiled=True,
    )
    portion = lax.all_gather(arrived, "tp", axis=2, tiled=True)
    flat_rows = portion.reshape(experts * capacity, portion.shape[2])
    gate_rows = gate_weight[0]
    up_rows = up_weight[0]
    gate_act = jnp.dot(flat_rows, gate_rows, preferred_element_type=jnp.float32)
    up_act = jnp.dot(flat_rows, up_rows, preferred_element_type=jnp.float32)
    hidden = (jax.nn.silu(gate_act) * up_act).astype(jnp.bfloat16)
    piece_sum = jnp.dot(hidden, down_weight[0], preferred_element_type=jnp.float32).astype(
        jnp.bfloat16
    )
    summed = (
        lax.psum_scatter(piece_sum, "tp", scatter_dimension=1, tiled=True)
        .astype(jnp.float32)
        .astype(jnp.bfloat16)
    )
    returned = lax.all_to_all(
        summed.reshape(experts, capacity, slice_width),
        "ep",
        split_axis=0,
        concat_axis=0,
        tiled=True,
    )
    returned = returned.reshape(experts * capacity, slice_width)
    copies = returned[target].astype(jnp.float32).reshape(tokens, choices_per, slice_width)
    expert_out = jnp.sum(copies * route_weight[..., None], axis=1).astype(jnp.bfloat16)
    return (mixer_out, expert_out)


def solution(mesh):
    placed = (
        P(("grp", "ep"), "tp"),
        P(("grp", "ep"), "tp"),
        P(("grp", "ep"), "tp"),
        P(("grp", "ep"), "tp"),
        P(("grp", "ep"), "tp"),
        P("tp"),
        P(None, "tp"),
        P(("grp", "ep"), None),
        P(),
        P(("grp", "ep"), None),
        P(("grp", "ep"), None),
        P("ep", None, "tp"),
        P("ep", None, "tp"),
        P("ep", "tp", None),
    )
    return jax.shard_map(
        on_device,
        mesh=mesh,
        in_specs=placed,
        out_specs=(P(("grp", "ep"), "tp"), P(("grp", "ep"), "tp")),
        check_vma=False,
    )
```
